32 devices in a mesh: ep: 4 (over y, x), tp: 8 (over z, core).
Axes of the slice: x: 2, y: 2, z: 4, core: 2. Of those that a mesh axis runs over, the one named last changes fastest.
Arguments:
- tokens: bfloat16 [128, 2048], P('ep', 'tp'), may hold values from -80 to 80
- delta_state: float32 [128, 16, 128, 128], P('ep', 'tp'), may hold values from -1.8 to 1.8
- mix_gain: bfloat16 [2048], replicated, may hold values from 0.099609375 to 1.8984375
- w_query: bfloat16 [2048, 2048], P(None, 'tp'), may hold values from -0.125 to 0.125
- w_key: bfloat16 [2048, 2048], P(None, 'tp'), may hold values from -0.125 to 0.125
- w_value: bfloat16 [2048, 2048], P(None, 'tp'), may hold values from -0.125 to 0.125
- w_outgate: bfloat16 [2048, 2048], P(None, 'tp'), may hold values from -0.125 to 0.125
- w_beta: bfloat16 [2048, 16], P(None, 'tp'), may hold values from -0.125 to 0.125
- w_decay: bfloat16 [2048, 16], P(None, 'tp'), may hold values from -0.125 to 0.125
- decay_scale: float32 [16], P('tp'), may hold values from 0.05 to 1.5
- decay_bias: float32 [16], P('tp'), may hold values from -1.5 to 1.5
- head_gain: bfloat16 [128], replicated, may hold values from 0.099609375 to 1.8984375
- w_output: bfloat16 [2048, 2048], P('tp'), may hold values from -0.125 to 0.125
- ffn_gain: bfloat16 [2048], replicated, may hold values from 0.099609375 to 1.8984375
- route_ids: int32 [128, 6], P('ep'), may hold values from 0 to 31, all different within a row; in each aligned block of 32 rows (0 to 31, 32 to 63, ...) at most 16 rows name the same one
- route_weights: float32 [128, 6], P('ep'), may hold values from 0.2 to 1.2
- expert_gate: bfloat16 [32, 2048, 512], P(('ep', 'tp')), may hold values from -0.125 to 0.125
- expert_up: bfloat16 [32, 2048, 512], P(('ep', 'tp')), may hold values from -0.125 to 0.125
- expert_down: bfloat16 [32, 512, 2048], P(('ep', 'tp')), may hold values from -0.25 to 0.25
- shared_gate: bfloat16 [2048, 512], P(None, 'tp'), may hold values from -0.125 to 0.125
- shared_up: bfloat16 [2048, 512], P(None, 'tp'), may hold values from -0.125 to 0.125
- shared_down: bfloat16 [512, 2048], P('tp'), may hold values from -0.25 to 0.25
Outputs:
- layer_out: bfloat16 [128, 2048], P('ep', 'tp')
- new_state: float32 [128, 16, 128, 128], P('ep', 'tp')
The draws below stay inside these ranges and needn't reach their ends.
Inputs may be any that keep to these rules, and one draw needn't show every extreme that they name: `route_ids`: each row names 6 different experts. In each aligned block of 32 rows (the sequences of one index of ep) no expert is named by more than 16 rows, and in every draw some expert is named by exactly 16 rows of some block.
All inputs are finite; a program needn't handle non-finite values.
Results may differ from the reference program's by a relative error of at most 0.013.
Values may be sent and summed in bfloat16 or wider, within the bound.
No kernel may reach another device: no remote copies, remote signals or barrier semaphores. Data moves between devices by JAX's collectives and lax.ppermute only.
A program may use at most 64 MiB of HBM per device.

```python
import math
import jax
import jax.numpy as jnp
import numpy as np
from jax import lax

D = 2048
HEADS = 16
DK = 128
DV = 128
FE = 512
FS = 512
TOP_K = 6
SEQ_GRP = 32
SEQS = 128
EXPERTS = 32
CAP = 16
N_EP = 4


def draw_tokens(key, part):
    subkeys = jax.random.split(key, 3)
    scale_low = 0.3
    scale_high = 3.0
    base_draw = jnp.clip(jax.random.normal(subkeys[0], (SEQS, D), jnp.float32), -6.0, 6.0)
    row_scales = jnp.exp(jax.random.uniform(subkeys[1], (SEQS, 1), jnp.float32, math.log(scale_low), math.log(scale_high)))
    col_scales = 3.0 ** (jnp.arange(D, dtype=jnp.float32) / D)
    col_scales = col_scales[None, :] * jax.random.uniform(subkeys[2], (1, D), jnp.float32, 0.6, 1.4)
    return (base_draw * row_scales * col_scales).astype(jnp.bfloat16)


def levels(own_key, shape, pieces, low, largest):
    def one(axis_at, shards_of):
        steps = jax.random.uniform(jax.random.fold_in(jax.random.fold_in(own_key, 6), axis_at), (shards_of,), jnp.float32, low / len(pieces), largest / len(pieces))
        return jnp.repeat(jnp.exp(steps), shape[axis_at] // shards_of).reshape((-1,) + (1,) * (len(shape) - axis_at - 1))

    gain = one(*pieces[0])
    for cut in pieces[1:]:
        gain = gain * one(*cut)
    return gain


def routed_block(own_key, own, number, rows, number_of, top, most, skew):
    sequence = jax.random.permutation(own_key, number_of)
    packed, common = portions_of(number_of, rows * top, most, skew, True), portions_of(number_of, rows * top, most, skew, False)
    places = jnp.arange(number_of)

    def named(sizes, offset_by):
        used = int((sizes > 0).sum())
        fixed = max(1, used // 4)
        passed = fixed + (places - fixed + offset_by * (used - fixed)) % max(1, number_of - fixed)
        return jnp.zeros((number_of,), jnp.int32).at[sequence[jnp.where(places < fixed, places, passed)]].set(jnp.asarray(sizes, jnp.int32))

    sizes = jnp.where(number % 4 == 0, named(packed, number // 4), named(common, number - number // 4 - 1))
    mixed = jax.random.permutation(jax.random.fold_in(own, 3), number_of)
    source_of, taker = mixed[0:number_of // 2 * 2:2], mixed[1:number_of // 2 * 2:2]
    slack = jnp.minimum(sizes[source_of] - 1, most - sizes[taker]) // 2
    slack = jnp.where((source_of == sequence[0]) | (taker == sequence[0]) | (sizes[taker] == 0), 0, jnp.maximum(slack, 0))
    passed = jax.random.randint(jax.random.fold_in(own, 4), (number_of // 2,), 0, 1 << 20) % (slack + 1)
    sizes = sizes.at[source_of].add(-passed).at[taker].add(passed)
    members = jnp.searchsorted(jnp.cumsum(sizes), jnp.arange(rows * top), side="right").astype(jnp.int32)
    listing = members.reshape(top, rows).T
    listing = listing[jax.random.permutation(jax.random.fold_in(own, 1), rows)]
    offset_by = jax.random.randint(jax.random.fold_in(own, 2), (rows, 1), 0, top)
    return jnp.take_along_axis(listing, (jnp.arange(top)[None, :] + offset_by) % top, axis=1)


def portions_of(number_of, total, most, skew, full):
    loads = [(1 << 20) // math.isqrt(rank ** skew) + 1 for rank in range(1, number_of + 1)]
    largest = most if full else min(most, max(-(-total // number_of), total * loads[0] // sum(loads)))
    least = 1 if total - largest >= number_of - 1 else 0
    given, surplus = [largest] + [least] * (number_of - 1), total - largest - least * (number_of - 1)
    while surplus > 0:
        movable = [i for i in range(1, number_of) if given[i] < largest] or [i for i in range(1, number_of) if given[i] < most]
        whole, budget = sum([loads[i] for i in movable]), surplus
        for i in movable:
            more = min(most - given[i], max(1, budget * loads[i] // whole), surplus)
            given[i] = given[i] + more
            surplus = surplus - more
    return np.array(given)


def centred(stream_key, extent, width, reach, pieces=(), kind=jnp.bfloat16):
    drawn = width * jax.random.normal(stream_key, extent, jnp.float32)
    if pieces:
        drawn = drawn * levels(stream_key, extent, pieces, -0.22, 0.18)
    return jnp.clip(drawn, -reach, reach).astype(kind)


def setup_inputs(seed: int = 0) -> dict:
    arg_keys = jax.random.split(jax.random.key(seed), 23)
    tokens = draw_tokens(jax.random.fold_in(arg_keys[22], 71), 0)
    delta_state = centred(arg_keys[1], (SEQS, HEADS, DK, DV), 0.3, 1.8, ((0, 4), (1, 8)), jnp.float32)
    mix_gain = jnp.clip(1.0 + 0.18 * jax.random.normal(arg_keys[2], (D,), jnp.float32), 0.099609375, 1.8984375).astype(jnp.bfloat16)
    w_query = centred(arg_keys[3], (D, HEADS * DK), D ** -0.5, 0.125, ((1, 8),))
    w_key = centred(arg_keys[4], (D, HEADS * DK), D ** -0.5, 0.125, ((1, 8),))
    w_value = centred(arg_keys[5], (D, HEADS * DV), D ** -0.5, 0.125, ((1, 8),))
    w_outgate = centred(arg_keys[6], (D, HEADS * DV), D ** -0.5, 0.125, ((1, 8),))
    w_beta = centred(arg_keys[7], (D, HEADS), D ** -0.5, 0.125, ((1, 8),))
    w_decay = centred(arg_keys[8], (D, HEADS), D ** -0.5, 0.125, ((1, 8),))
    decay_scale = jnp.clip(jnp.exp(math.log(1.5) - 3.4011974 * jax.random.uniform(arg_keys[9], (HEADS,), jnp.float32) ** levels(arg_keys[9], (HEADS,), ((0, 8),), -0.2, 0.2)), 0.05, 1.5)
    decay_bias = jnp.clip(jax.random.uniform(arg_keys[10], (HEADS,), jnp.float32, -1.5, 1.5) * levels(arg_keys[10], (HEADS,), ((0, 8),), -0.4, 0.0), -1.5, 1.5)
    head_gain = jnp.clip(1.0 + 0.18 * jax.random.normal(arg_keys[11], (DV,), jnp.float32), 0.099609375, 1.8984375).astype(jnp.bfloat16)
    w_output = centred(arg_keys[12], (HEADS * DV, D), (HEADS * DV) ** -0.5, 0.125, ((0, 8),))
    ffn_gain = jnp.clip(1.0 + 0.18 * jax.random.normal(arg_keys[13], (D,), jnp.float32), 0.099609375, 1.8984375).astype(jnp.bfloat16)
    route_ids_keys = jax.random.split(jax.random.fold_in(arg_keys[14], 1), SEQS // SEQ_GRP)
    route_ids_turns = jax.random.permutation(jax.random.fold_in(arg_keys[14], 3), SEQS // SEQ_GRP)
    route_ids = jax.vmap(lambda own, number: routed_block(jax.random.fold_in(arg_keys[14], 2), own, number, SEQ_GRP, EXPERTS, TOP_K, CAP, 2))(route_ids_keys, route_ids_turns).reshape((SEQS, TOP_K))
    route_weights = jnp.clip(0.2 + 1 * jax.random.uniform(arg_keys[15], (SEQS, TOP_K), jnp.float32) ** levels(arg_keys[15], (SEQS, TOP_K), ((0, 4),), -0.2, 0.2), 0.2, 1.2)
    expert_gate = centred(arg_keys[16], (EXPERTS, D, FE), D ** -0.5, 0.125, ((0, 32),))
    expert_up = centred(arg_keys[17], (EXPERTS, D, FE), D ** -0.5, 0.125, ((0, 32),))
    expert_down = centred(arg_keys[18], (EXPERTS, FE, D), FE ** -0.5, 0.25, ((0, 32),))
    shared_gate = centred(arg_keys[19], (D, FS), D ** -0.5, 0.125, ((1, 8),))
    shared_up = centred(arg_keys[20], (D, FS), D ** -0.5, 0.125, ((1, 8),))
    shared_down = centred(arg_keys[21], (FS, D), FS ** -0.5, 0.25, ((0, 8),))
    return {"tokens": tokens, "delta_state": delta_state, "mix_gain": mix_gain, "w_query": w_query, "w_key": w_key, "w_value": w_value, "w_outgate": w_outgate, "w_beta": w_beta, "w_decay": w_decay, "decay_scale": decay_scale, "decay_bias": decay_bias, "head_gain": head_gain, "w_output": w_output, "ffn_gain": ffn_gain, "route_ids": route_ids, "route_weights": route_weights, "expert_gate": expert_gate, "expert_up": expert_up, "expert_down": expert_down, "shared_gate": shared_gate, "shared_up": shared_up, "shared_down": shared_down}


epsilon = 1e-06

def rms_norm(values, gain_vector):
    squares = lax.optimization_barrier(jnp.mean(values * values, axis=-1, keepdims=True))
    return values * lax.rsqrt(squares + epsilon) * gain_vector.astype(jnp.float32)

def unit_rows(values):
    return values * lax.rsqrt(lax.optimization_barrier(jnp.sum(values * values, axis=-1, keepdims=True)) + epsilon)

def reference(tokens, delta_state, mix_gain, w_query, w_key, w_value, w_outgate, w_beta, w_decay, decay_scale, decay_bias, head_gain, w_output, ffn_gain, route_ids, route_weights, expert_gate, expert_up, expert_down, shared_gate, shared_up, shared_down):
    rows_count = tokens.shape[0]
    resid_in = tokens.astype(jnp.float32)
    normed_mix = rms_norm(resid_in, mix_gain).astype(jnp.bfloat16)

    def project(weight):
        result = jnp.dot(normed_mix, weight, preferred_element_type=jnp.float32)
        result = lax.optimization_barrier(result.astype(jnp.bfloat16)).astype(jnp.float32)
        return result.reshape(rows_count, HEADS, -1)
    query_unit = unit_rows(project(w_query)) * DK ** (-0.5)
    key_unit = unit_rows(project(w_key))
    values_new = project(w_value)
    out_gate = project(w_outgate)
    beta_gate = jax.nn.sigmoid(jnp.dot(normed_mix, w_beta, preferred_element_type=jnp.float32))
    decay_input = jnp.dot(normed_mix, w_decay, preferred_element_type=jnp.float32) + decay_bias
    decay_rate = jnp.exp(-decay_scale * jax.nn.softplus(decay_input))
    key_read = jnp.einsum('shk,shkv->shv', key_unit, delta_state)
    written = beta_gate[:, :, None] * key_unit
    kept_state = delta_state - written[:, :, :, None] * key_read[:, :, None, :]
    new_state = decay_rate[:, :, None, None] * kept_state + written[:, :, :, None] * values_new[:, :, None, :]
    state_read = jnp.einsum('shk,shkv->shv', query_unit, new_state)
    gated = (rms_norm(state_read, head_gain) * jax.nn.silu(out_gate)).reshape(rows_count, -1).astype(jnp.bfloat16)
    resid_mid = resid_in + jnp.dot(gated, w_output, preferred_element_type=jnp.float32)
    normed_ffn = rms_norm(resid_mid, ffn_gain).astype(jnp.bfloat16)
    pair_count = rows_count * TOP_K
    flat_ids = route_ids.reshape(pair_count).astype(jnp.int32)
    flat_rows = (jnp.arange(pair_count, dtype=jnp.int32) // TOP_K).astype(jnp.int32)
    flat_weights = route_weights.reshape(pair_count)
    sorted_order = jnp.argsort(flat_ids, stable=True).astype(jnp.int32)
    sorted_ids = flat_ids[sorted_order]
    expert_range = jnp.arange(EXPERTS, dtype=jnp.int32)
    starts = jnp.searchsorted(sorted_ids, expert_range, side='left').astype(jnp.int32)
    finish = jnp.searchsorted(sorted_ids, expert_range, side='right').astype(jnp.int32)
    most_rows = N_EP * CAP

    def one_expert(running, expert):
        places = starts[expert] + jnp.arange(most_rows, dtype=jnp.int32)
        in_range = places < finish[expert]
        chosen = sorted_order[jnp.minimum(places, pair_count - 1).astype(jnp.int32)]
        rows_at = flat_rows[chosen]
        weights_at = jnp.where(in_range, flat_weights[chosen], 0.0)
        inputs = normed_ffn[rows_at]
        gate_part = jnp.dot(inputs, expert_gate[expert], preferred_element_type=jnp.float32)
        up_part = jnp.dot(inputs, expert_up[expert], preferred_element_type=jnp.float32)
        hidden = (jax.nn.silu(gate_part) * up_part).astype(jnp.bfloat16)
        outputs = jnp.dot(hidden, expert_down[expert], preferred_element_type=jnp.float32)
        outputs = lax.optimization_barrier(outputs.astype(jnp.bfloat16)).astype(jnp.float32)
        return (running.at[rows_at].add(weights_at[:, None] * outputs), None)
    routed, _ = lax.scan(one_expert, jnp.zeros((rows_count, D), jnp.float32), expert_range)
    shared_gate_part = jnp.dot(normed_ffn, shared_gate, preferred_element_type=jnp.float32)
    shared_up_part = jnp.dot(normed_ffn, shared_up, preferred_element_type=jnp.float32)
    hidden_shared = (jax.nn.silu(shared_gate_part) * shared_up_part).astype(jnp.bfloat16)
    shared_out = jnp.dot(hidden_shared, shared_down, preferred_element_type=jnp.float32)
    layer_out = (resid_mid + routed + shared_out).astype(jnp.bfloat16)
    return (layer_out, new_state)
```

```python
import jax
import jax.numpy as jnp
from jax import lax
from jax.experimental import pallas as pl
from jax.experimental.pallas import tpu as pltpu
from jax.sharding import PartitionSpec as P

epsilon = 1e-06


def rms_norm(values, gain_vector):
    squares = jnp.mean(values * values, axis=-1, keepdims=True)
    return values * lax.rsqrt(squares + epsilon) * gain_vector.astype(jnp.float32)


def unit_rows(values):
    return values * lax.rsqrt(jnp.sum(values * values, axis=-1, keepdims=True) + epsilon)


def other_core(count):
    return [(index, index ^ 1) for index in range(count)]


def chip_groups(count):
    return [list(range(core, count, 2)) for core in range(2)]


def exchange_chips(blocks):
    count = lax.axis_size("tp")
    return lax.all_to_all(
        blocks, "tp", 0, 0, tiled=True, axis_index_groups=chip_groups(count)
    )


def swap_cores(block):
    return lax.ppermute(block, "tp", other_core(lax.axis_size("tp")))


def pair_sum(partial, core):
    count = lax.axis_size("tp")
    rows, columns = partial.shape
    blocks = partial.reshape(rows, count // 2, 2, columns // count).transpose(2, 1, 0, 3)
    kept = jnp.where(core == 0, blocks[0], blocks[1])
    sent = jnp.where(core == 0, blocks[1], blocks[0]).astype(jnp.bfloat16)
    return (kept + swap_cores(sent).astype(jnp.float32)).astype(jnp.bfloat16)


def scatter_sum(partial, core):
    received = exchange_chips(pair_sum(partial, core))
    return jnp.sum(received.astype(jnp.float32), axis=0)


def sum_chips(halves):
    chips = halves.shape[0]
    copies = jnp.broadcast_to(halves[None], (chips,) + halves.shape)
    received = exchange_chips(copies.reshape((chips * chips,) + halves.shape[1:]))
    received = received.reshape((chips,) + halves.shape).astype(jnp.float32)
    return jnp.sum(received, axis=0).astype(jnp.bfloat16)


def expert_block(rows, expert_gate, expert_up, expert_down):
    gate_part = jnp.einsum("sjnd,jdf->sjnf", rows, expert_gate, preferred_element_type=jnp.float32)
    up_part = jnp.einsum("sjnd,jdf->sjnf", rows, expert_up, preferred_element_type=jnp.float32)
    hidden = (jax.nn.silu(gate_part) * up_part).astype(jnp.bfloat16)
    outputs = jnp.einsum("sjnf,jfd->sjnd", hidden, expert_down, preferred_element_type=jnp.float32)
    return outputs.astype(jnp.bfloat16)


def ordered(own_ref, theirs_ref, chip, core):
    own = own_ref[chip].astype(jnp.float32)
    theirs = theirs_ref[chip].astype(jnp.float32)
    return [jnp.where(core == 0, own, theirs), jnp.where(core == 0, theirs, own)]


def split_store(full, width, core, kept_ref, sent_ref):
    for chip in range(kept_ref.shape[0]):
        first = full[:, 2 * chip * width : (2 * chip + 1) * width]
        second = full[:, (2 * chip + 1) * width : (2 * chip + 2) * width]
        kept_ref[chip] = jnp.where(core == 0, first, second)
        sent_ref[chip] = jnp.where(core == 0, second, first).astype(jnp.bfloat16)


def mixer_kernel(
    place_ref, scale_ref, bias_ref, own_ref, theirs_ref, gain_ref, beta_ref, decay_ref, head_gain_ref,
    query_hbm, key_hbm, value_hbm, gate_hbm, output_hbm, state_hbm,
    new_hbm, kept_ref, sent_ref, rows_ref,
    weights, output_weight, state, sems,
):
    core = place_ref[0] % 2
    rows_count, heads_here, key_size, value_size = state.shape
    chips, _, width = own_ref.shape
    group = 8
    chunks = rows_count // group
    weight_copies = [
        pltpu.make_async_copy(source, weights.at[index], sems.at[index])
        for index, source in enumerate((key_hbm, query_hbm, value_hbm, gate_hbm))
    ]
    output_copy = pltpu.make_async_copy(output_hbm, output_weight, sems.at[4])
    reads = [
        pltpu.make_async_copy(
            state_hbm.at[pl.ds(group * c, group)], state.at[pl.ds(group * c, group)], sems.at[5 + c]
        )
        for c in range(chunks)
    ]
    writes = [
        pltpu.make_async_copy(
            state.at[pl.ds(group * c, group)],
            new_hbm.at[pl.ds(group * c, group)],
            sems.at[5 + chunks + c],
        )
        for c in range(chunks)
    ]
    for copy in weight_copies[:3] + reads + [weight_copies[3], output_copy]:
        copy.start()
    pieces = []
    for chip in range(chips):
        pieces += ordered(own_ref, theirs_ref, chip, core)
    resid = jnp.concatenate(pieces, axis=1)
    rows_ref[...] = resid.astype(jnp.bfloat16)
    normed_wide = rms_norm(resid, gain_ref[...])
    normed = normed_wide.astype(jnp.bfloat16)
    normed_wide = normed.astype(jnp.float32)

    def project(index):
        weight_copies[index].wait()
        result = jnp.dot(normed, weights[index], preferred_element_type=jnp.float32)
        return result.astype(jnp.bfloat16).astype(jnp.float32)

    betas, decays = [], []
    for head in range(heads_here):
        beta_in = jnp.sum(
            normed_wide * beta_ref[head : head + 1, :].astype(jnp.float32), axis=1, keepdims=True
        )
        decay_in = jnp.sum(
            normed_wide * decay_ref[head : head + 1, :].astype(jnp.float32), axis=1, keepdims=True
        ) + bias_ref[head]
        soft = jnp.maximum(decay_in, 0.0) + jnp.log1p(jnp.exp(-jnp.abs(decay_in)))
        betas.append(1.0 / (1.0 + jnp.exp(-beta_in)))
        decays.append(jnp.broadcast_to(jnp.exp(-scale_ref[head] * soft), (rows_count, value_size)))
    keys_all = project(0)
    queries_all = project(1)
    values_all = project(2)
    heads = range(heads_here)
    cut = lambda array, head, size: array[:, head * size : (head + 1) * size]
    keys = [unit_rows(cut(keys_all, head, key_size)) for head in heads]
    queries = [unit_rows(cut(queries_all, head, key_size)) * key_size ** (-0.5) for head in heads]
    values = [cut(values_all, head, value_size) for head in heads]
    mixes = [jnp.sum(keys[head] * queries[head], axis=1, keepdims=True) for head in heads]
    key_columns = [keys[head].T for head in heads]
    query_columns = [queries[head].T for head in heads]
    state_reads = [[] for _ in heads]
    for c in range(chunks):
        reads[c].wait()
        low, high = group * c, group * (c + 1)
        for head in heads:
            key_parts, query_parts = [], []
            for s in range(low, high):
                old = state[s, head]
                key_parts.append(
                    jnp.sum(old * key_columns[head][:, s : s + 1], axis=0, keepdims=True)
                )
                query_parts.append(
                    jnp.sum(old * query_columns[head][:, s : s + 1], axis=0, keepdims=True)
                )
            decay = decays[head][low:high]
            change = betas[head][low:high] * (
                values[head][low:high] - decay * jnp.concatenate(key_parts, axis=0)
            )
            state_reads[head].append(
                decay * jnp.concatenate(query_parts, axis=0) + mixes[head][low:high] * change
            )
            for s in range(low, high):
                at = s - low
                state[s, head] = (
                    decay[at : at + 1] * state[s, head]
                    + key_columns[head][:, s : s + 1] * change[at : at + 1]
                )
        writes[c].start()
    gates_all = project(3)
    gated = []
    for head in heads:
        gate = cut(gates_all, head, value_size)
        normal = rms_norm(jnp.concatenate(state_reads[head], axis=0), head_gain_ref[...])
        gated.append((normal * (gate / (1.0 + jnp.exp(-gate)))).astype(jnp.bfloat16))
    output_copy.wait()
    partial = jnp.dot(
        jnp.concatenate(gated, axis=1), output_weight[...], preferred_element_type=jnp.float32
    )
    split_store(partial, width, core, kept_ref, sent_ref)
    for copy in writes:
        copy.wait()


def mixer(place, own, theirs, delta_state, mix_gain, w_query, w_key, w_value, w_outgate, w_beta,
          w_decay, decay_scale, decay_bias, head_gain, w_output):
    chips, rows_count, width = own.shape
    columns = w_query.shape[0]
    vmem = pl.BlockSpec(memory_space=pltpu.VMEM)
    smem = pl.BlockSpec(memory_space=pltpu.SMEM)
    hbm = pl.BlockSpec(memory_space=pltpu.HBM)
    return pl.pallas_call(
        mixer_kernel,
        name="mixer",
        in_specs=[smem] * 3 + [vmem] * 6 + [hbm] * 6,
        out_specs=[hbm, vmem, vmem, vmem],
        out_shape=[
            pltpu.HBM(delta_state.shape, jnp.float32),
            jax.ShapeDtypeStruct((chips, rows_count, width), jnp.float32),
            jax.ShapeDtypeStruct((chips, rows_count, width), jnp.bfloat16),
            jax.ShapeDtypeStruct((rows_count, columns), jnp.bfloat16),
        ],
        scratch_shapes=[
            pltpu.VMEM((4,) + w_query.shape, jnp.bfloat16),
            pltpu.VMEM(w_output.shape, jnp.bfloat16),
            pltpu.VMEM(delta_state.shape, jnp.float32),
            pltpu.SemaphoreType.DMA((5 + 2 * (rows_count // 8),)),
        ],
        compiler_params=pltpu.CompilerParams(vmem_limit_bytes=40 * 2**20),
    )(
        place, decay_scale, decay_bias, own, theirs, mix_gain[None], w_beta.T, w_decay.T,
        head_gain[None],
        *[pltpu.with_memory_space_constraint(array, pltpu.HBM)
          for array in (w_query, w_key, w_value, w_outgate, w_output, delta_state)],
    )


def dispatch_kernel(
    place_ref, own_ref, theirs_ref, rows_ref, gain_ref, choose_ref, outgoing_ref, normed_ref, resid_ref
):
    core = place_ref[0] % 2
    chips, _, width = own_ref.shape
    pieces = []
    for chip in range(chips):
        pieces += ordered(own_ref, theirs_ref, chip, core)
    resid = jnp.concatenate(pieces, axis=1) + rows_ref[...].astype(jnp.float32)
    normed = rms_norm(resid, gain_ref[...]).astype(jnp.bfloat16)
    normed_ref[...] = normed
    outgoing = jnp.dot(choose_ref[...], normed, preferred_element_type=jnp.float32)
    outgoing_ref[...] = outgoing.astype(jnp.bfloat16)
    here = jnp.zeros(resid_ref.shape, jnp.float32)
    for block in range(2 * chips):
        here = jnp.where(place_ref[0] == block, resid[:, block * width : (block + 1) * width], here)
    resid_ref[...] = here


def dispatch(place, own, theirs, rows, gain, choose):
    vmem = pl.BlockSpec(memory_space=pltpu.VMEM)
    smem = pl.BlockSpec(memory_space=pltpu.SMEM)
    return pl.pallas_call(
        dispatch_kernel,
        name="dispatch",
        in_specs=[smem] + [vmem] * 5,
        out_specs=[vmem] * 3,
        out_shape=[
            jax.ShapeDtypeStruct((choose.shape[0], rows.shape[1]), jnp.bfloat16),
            jax.ShapeDtypeStruct(rows.shape, jnp.bfloat16),
            jax.ShapeDtypeStruct(own.shape[1:], jnp.float32),
        ],
    )(place, own, theirs, rows, gain[None], choose)


def body(
    tokens,
    delta_state,
    mix_gain,
    w_query,
    w_key,
    w_value,
    w_outgate,
    w_beta,
    w_decay,
    decay_scale,
    decay_bias,
    head_gain,
    w_output,
    ffn_gain,
    route_ids,
    route_weights,
    expert_gate,
    expert_up,
    expert_down,
    shared_gate,
    shared_up,
    shared_down,
):
    rows_count = tokens.shape[0]
    heads_here = delta_state.shape[1]
    tp_index = lax.axis_index("tp")
    core = tp_index % 2
    place = tp_index[None]
    chips = lax.axis_size("tp") // 2
    own_rows = exchange_chips(jnp.broadcast_to(tokens[None], (chips,) + tokens.shape))
    new_state, kept, sent, full_rows = mixer(
        place, own_rows, swap_cores(own_rows), delta_state, mix_gain, w_query, w_key, w_value,
        w_outgate, w_beta, w_decay, decay_scale, decay_bias, head_gain, w_output,
    )
    halves = (kept + swap_cores(sent).astype(jnp.float32)).astype(jnp.bfloat16)
    mixed = sum_chips(halves)
    model_width = full_rows.shape[1]
    ep_count = lax.axis_size("ep")
    tp_count = lax.axis_size("tp")
    experts_here = expert_gate.shape[0]
    top_count = route_ids.shape[1]
    expert_total = experts_here * ep_count * tp_count
    capacity = max(2, 8 * rows_count * top_count // (3 * expert_total))
    pair_count = rows_count * top_count
    flat_ids = route_ids.reshape(pair_count)
    owner_ep = flat_ids // (tp_count * experts_here)
    owner_tp = flat_ids // experts_here % tp_count
    local_slot = flat_ids % experts_here
    mine_mask = owner_tp == tp_index
    pair_weights = jnp.where(mine_mask, route_weights.reshape(pair_count), 0.0)
    pair_index = jnp.arange(pair_count, dtype=jnp.int32)
    earlier = (flat_ids[:, None] == flat_ids[None, :]) & (pair_index[None, :] < pair_index[:, None])
    slot_rank = jnp.sum(earlier.astype(jnp.int32), axis=1)
    slot_count = ep_count * experts_here * capacity
    target = jnp.where(mine_mask, (owner_ep * experts_here + local_slot) * capacity + slot_rank, -1)
    choose = (target[:, None] == jnp.arange(slot_count, dtype=jnp.int32)[None, :]).astype(
        jnp.bfloat16
    )
    by_row = jnp.sum(choose.reshape(rows_count, top_count, slot_count), axis=1)
    outgoing, normed_ffn, resid_own = dispatch(
        place, mixed, swap_cores(mixed), full_rows, ffn_gain, by_row.T
    )
    outgoing = outgoing.reshape(ep_count, experts_here, capacity, model_width)
    results = expert_block(
        lax.all_to_all(outgoing, "ep", split_axis=0, concat_axis=0, tiled=True),
        expert_gate,
        expert_up,
        expert_down,
    )
    returned = lax.all_to_all(results, "ep", split_axis=0, concat_axis=0, tiled=True)
    weights_of = jnp.sum(
        jnp.where(choose > 0, pair_weights[:, None], 0.0).reshape(rows_count, top_count, slot_count),
        axis=1,
    )
    weights_high = weights_of.astype(jnp.bfloat16)
    weights_low = (weights_of - weights_high.astype(jnp.float32)).astype(jnp.bfloat16)
    returned = returned.reshape(slot_count, model_width)
    routed = jnp.dot(
        jnp.concatenate([weights_high, weights_low], axis=1),
        jnp.concatenate([returned, returned], axis=0),
        preferred_element_type=jnp.float32,
    )
    shared_gate_part = jnp.dot(normed_ffn, shared_gate, preferred_element_type=jnp.float32)
    shared_up_part = jnp.dot(normed_ffn, shared_up, preferred_element_type=jnp.float32)
    hidden_shared = (jax.nn.silu(shared_gate_part) * shared_up_part).astype(jnp.bfloat16)
    branch_sum = routed + jnp.dot(hidden_shared, shared_down, preferred_element_type=jnp.float32)
    combined = scatter_sum(branch_sum, core)
    layer_out = (resid_own + combined).astype(jnp.bfloat16)
    return (layer_out, new_state)


def solution(mesh):
    return jax.shard_map(
        body,
        mesh=mesh,
        in_specs=(
            P("ep", "tp"),
            P("ep", "tp", None, None),
            P(),
            P(None, "tp"),
            P(None, "tp"),
            P(None, "tp"),
            P(None, "tp"),
            P(None, "tp"),
            P(None, "tp"),
            P("tp"),
            P("tp"),
            P(),
            P("tp", None),
            P(),
            P("ep", None),
            P("ep", None),
            P(("ep", "tp"), None, None),
            P(("ep", "tp"), None, None),
            P(("ep", "tp"), None, None),
            P(None, "tp"),
            P(None, "tp"),
            P("tp", None),
        ),
        out_specs=(P("ep", "tp"), P("ep", "tp", None, None)),
        check_vma=False,
    )
```

```python
import jax
import jax.numpy as jnp
from jax import lax
from jax.experimental import pallas as pl
from jax.experimental.pallas import tpu as pltpu
from jax.sharding import PartitionSpec as P

epsilon = 1e-06


def rms_norm(values, gain_vector):
    squares = jnp.mean(values * values, axis=-1, keepdims=True)
    return values * lax.rsqrt(squares + epsilon) * gain_vector.astype(jnp.float32)


def unit_rows(values):
    return values * lax.rsqrt(jnp.sum(values * values, axis=-1, keepdims=True) + epsilon)


def other_core(count):
    return [(index, index ^ 1) for index in range(count)]


def chip_groups(count):
    return [list(range(core, count, 2)) for core in range(2)]


def exchange_chips(blocks):
    count = lax.axis_size("tp")
    return lax.all_to_all(
        blocks, "tp", 0, 0, tiled=True, axis_index_groups=chip_groups(count)
    )


def swap_cores(block):
    return lax.ppermute(block, "tp", other_core(lax.axis_size("tp")))


def pair_sum(partial, core):
    count = lax.axis_size("tp")
    rows, columns = partial.shape
    blocks = partial.reshape(rows, count // 2, 2, columns // count).transpose(2, 1, 0, 3)
    kept = jnp.where(core == 0, blocks[0], blocks[1])
    sent = jnp.where(core == 0, blocks[1], blocks[0]).astype(jnp.bfloat16)
    return (kept + swap_cores(sent).astype(jnp.float32)).astype(jnp.bfloat16)


def scatter_sum(partial, core):
    received = exchange_chips(pair_sum(partial, core))
    return jnp.sum(received.astype(jnp.float32), axis=0)


def sum_chips(halves):
    chips = halves.shape[0]
    copies = jnp.broadcast_to(halves[None], (chips,) + halves.shape)
    received = exchange_chips(copies.reshape((chips * chips,) + halves.shape[1:]))
    received = received.reshape((chips,) + halves.shape).astype(jnp.float32)
    return jnp.sum(received, axis=0).astype(jnp.bfloat16)


def expert_block(rows, expert_gate, expert_up, expert_down):
    gate_part = jnp.einsum("sjnd,jdf->sjnf", rows, expert_gate, preferred_element_type=jnp.float32)
    up_part = jnp.einsum("sjnd,jdf->sjnf", rows, expert_up, preferred_element_type=jnp.float32)
    hidden = (jax.nn.silu(gate_part) * up_part).astype(jnp.bfloat16)
    outputs = jnp.einsum("sjnf,jfd->sjnd", hidden, expert_down, preferred_element_type=jnp.float32)
    return outputs.astype(jnp.bfloat16)


def ordered(own_ref, theirs_ref, chip, core):
    own = own_ref[chip].astype(jnp.float32)
    theirs = theirs_ref[chip].astype(jnp.float32)
    return [jnp.where(core == 0, own, theirs), jnp.where(core == 0, theirs, own)]


def split_store(full, width, core, kept_ref, sent_ref):
    for chip in range(kept_ref.shape[0]):
        first = full[:, 2 * chip * width : (2 * chip + 1) * width]
        second = full[:, (2 * chip + 1) * width : (2 * chip + 2) * width]
        kept_ref[chip] = jnp.where(core == 0, first, second)
        sent_ref[chip] = jnp.where(core == 0, second, first).astype(jnp.bfloat16)


def mixer_kernel(
    place_ref, own_ref, theirs_ref, small_ref,
    query_hbm, key_hbm, value_hbm, gate_hbm, output_hbm, state_hbm,
    new_hbm, kept_ref, sent_ref, rows_ref,
    weights, output_weight, state, sems,
):
    core = place_ref[0] % 2
    rows_count, heads_here, key_size, value_size = state.shape
    chips, _, width = own_ref.shape
    group = 8
    chunks = rows_count // group
    weight_copies = [
        pltpu.make_async_copy(source, weights.at[index], sems.at[index])
        for index, source in enumerate((key_hbm, query_hbm, value_hbm, gate_hbm))
    ]
    output_copy = pltpu.make_async_copy(output_hbm, output_weight, sems.at[4])
    reads = [
        pltpu.make_async_copy(
            state_hbm.at[pl.ds(group * c, group)], state.at[pl.ds(group * c, group)], sems.at[5 + c]
        )
        for c in range(chunks)
    ]
    writes = [
        pltpu.make_async_copy(
            state.at[pl.ds(group * c, group)],
            new_hbm.at[pl.ds(group * c, group)],
            sems.at[5 + chunks + c],
        )
        for c in range(chunks)
    ]
    for copy in weight_copies[:3] + reads + [weight_copies[3], output_copy]:
        copy.start()
    pieces = []
    for chip in range(chips):
        pieces += ordered(own_ref, theirs_ref, chip, core)
    resid = jnp.concatenate(pieces, axis=1)
    rows_ref[...] = resid.astype(jnp.bfloat16)
    small = lambda row, size: small_ref[row : row + 1, :size]
    vectors = 2 * heads_here
    normed = rms_norm(resid, small_ref[vectors : vectors + 1, :]).astype(jnp.bfloat16)
    normed_wide = normed.astype(jnp.float32)

    def project(index):
        weight_copies[index].wait()
        result = jnp.dot(normed, weights[index], preferred_element_type=jnp.float32)
        return result.astype(jnp.bfloat16).astype(jnp.float32)

    betas, decays = [], []
    for head in range(heads_here):
        beta_in = jnp.sum(
            normed_wide * small_ref[head : head + 1, :], axis=1, keepdims=True
        )
        decay_in = jnp.sum(
            normed_wide * small_ref[heads_here + head : heads_here + head + 1, :],
            axis=1,
            keepdims=True,
        ) + small_ref[vectors + 3 : vectors + 4, head : head + 1]
        soft = jnp.maximum(decay_in, 0.0) + jnp.log1p(jnp.exp(-jnp.abs(decay_in)))
        betas.append(1.0 / (1.0 + jnp.exp(-beta_in)))
        decays.append(jnp.broadcast_to(jnp.exp(-small_ref[vectors + 2 : vectors + 3, head : head + 1] * soft), (rows_count, value_size)))
    keys_all = project(0)
    queries_all = project(1)
    values_all = project(2)
    heads = range(heads_here)
    cut = lambda array, head, size: array[:, head * size : (head + 1) * size]
    keys = [unit_rows(cut(keys_all, head, key_size)) for head in heads]
    queries = [unit_rows(cut(queries_all, head, key_size)) * key_size ** (-0.5) for head in heads]
    values = [cut(values_all, head, value_size) for head in heads]
    mixes = [jnp.sum(keys[head] * queries[head], axis=1, keepdims=True) for head in heads]
    key_columns = [keys[head].T for head in heads]
    query_columns = [queries[head].T for head in heads]
    state_reads = [[] for _ in heads]
    for c in range(chunks):
        reads[c].wait()
        low, high = group * c, group * (c + 1)
        for head in heads:
            key_parts, query_parts = [], []
            for s in range(low, high):
                old = state[s, head]
                key_parts.append(
                    jnp.sum(old * key_columns[head][:, s : s + 1], axis=0, keepdims=True)
                )
                query_parts.append(
                    jnp.sum(old * query_columns[head][:, s : s + 1], axis=0, keepdims=True)
                )
            decay = decays[head][low:high]
            change = betas[head][low:high] * (
                values[head][low:high] - decay * jnp.concatenate(key_parts, axis=0)
            )
            state_reads[head].append(
                decay * jnp.concatenate(query_parts, axis=0) + mixes[head][low:high] * change
            )
            for s in range(low, high):
                at = s - low
                state[s, head] = (
                    decay[at : at + 1] * state[s, head]
                    + key_columns[head][:, s : s + 1] * change[at : at + 1]
                )
        writes[c].start()
    gates_all = project(3)
    gated = []
    for head in heads:
        gate = cut(gates_all, head, value_size)
        normal = rms_norm(jnp.concatenate(state_reads[head], axis=0), small(vectors + 1, value_size))
        gated.append((normal * (gate / (1.0 + jnp.exp(-gate)))).astype(jnp.bfloat16))
    output_copy.wait()
    partial = jnp.dot(
        jnp.concatenate(gated, axis=1), output_weight[...], preferred_element_type=jnp.float32
    )
    split_store(partial, width, core, kept_ref, sent_ref)
    for copy in writes:
        copy.wait()


def pack_small(w_beta, w_decay, mix_gain, head_gain, decay_scale, decay_bias, ffn_gain):
    columns = w_beta.shape[0]
    row = lambda v: jnp.pad(v.astype(jnp.float32), (0, columns - v.shape[0]))[None]
    vectors = (mix_gain, head_gain, decay_scale, decay_bias, ffn_gain)
    rows = [w_beta.T.astype(jnp.float32), w_decay.T.astype(jnp.float32)] + [row(v) for v in vectors]
    return jnp.concatenate(rows, axis=0)


def mixer(place, own, theirs, small, delta_state, w_query, w_key, w_value, w_outgate, w_output):
    chips, rows_count, width = own.shape
    columns = w_query.shape[0]
    vmem = pl.BlockSpec(memory_space=pltpu.VMEM)
    smem = pl.BlockSpec(memory_space=pltpu.SMEM)
    hbm = pl.BlockSpec(memory_space=pltpu.HBM)
    return pl.pallas_call(
        mixer_kernel,
        name="mixer",
        in_specs=[smem] + [vmem] * 3 + [hbm] * 6,
        out_specs=[hbm, vmem, vmem, vmem],
        out_shape=[
            pltpu.HBM(delta_state.shape, jnp.float32),
            jax.ShapeDtypeStruct((chips, rows_count, width), jnp.float32),
            jax.ShapeDtypeStruct((chips, rows_count, width), jnp.bfloat16),
            jax.ShapeDtypeStruct((rows_count, columns), jnp.bfloat16),
        ],
        scratch_shapes=[
            pltpu.VMEM((4,) + w_query.shape, jnp.bfloat16),
            pltpu.VMEM(w_output.shape, jnp.bfloat16),
            pltpu.VMEM(delta_state.shape, jnp.float32),
            pltpu.SemaphoreType.DMA((5 + 2 * (rows_count // 8),)),
        ],
        compiler_params=pltpu.CompilerParams(vmem_limit_bytes=40 * 2**20),
    )(
        place, own, theirs, small,
        *[pltpu.with_memory_space_constraint(array, pltpu.HBM)
          for array in (w_query, w_key, w_value, w_outgate, w_output, delta_state)],
    )


def dispatch_kernel(
    place_ref, own_ref, theirs_ref, rows_ref, gain_ref, choose_ref, outgoing_ref, normed_ref, resid_ref
):
    core = place_ref[0] % 2
    chips, _, width = own_ref.shape
    pieces = []
    for chip in range(chips):
        pieces += ordered(own_ref, theirs_ref, chip, core)
    resid = jnp.concatenate(pieces, axis=1) + rows_ref[...].astype(jnp.float32)
    normed = rms_norm(resid, gain_ref[gain_ref.shape[0] - 1 :, :]).astype(jnp.bfloat16)
    normed_ref[...] = normed
    outgoing = jnp.dot(choose_ref[...], normed, preferred_element_type=jnp.float32)
    outgoing_ref[...] = outgoing.astype(jnp.bfloat16)
    here = jnp.zeros(resid_ref.shape, jnp.float32)
    for block in range(2 * chips):
        here = jnp.where(place_ref[0] == block, resid[:, block * width : (block + 1) * width], here)
    resid_ref[...] = here


def dispatch(place, own, theirs, rows, gain, choose):
    vmem = pl.BlockSpec(memory_space=pltpu.VMEM)
    smem = pl.BlockSpec(memory_space=pltpu.SMEM)
    return pl.pallas_call(
        dispatch_kernel,
        name="dispatch",
        in_specs=[smem] + [vmem] * 5,
        out_specs=[vmem] * 3,
        out_shape=[
            jax.ShapeDtypeStruct((choose.shape[0], rows.shape[1]), jnp.bfloat16),
            jax.ShapeDtypeStruct(rows.shape, jnp.bfloat16),
            jax.ShapeDtypeStruct(own.shape[1:], jnp.float32),
        ],
    )(place, own, theirs, rows, gain, choose)


def body(
    tokens,
    delta_state,
    mix_gain,
    w_query,
    w_key,
    w_value,
    w_outgate,
    w_beta,
    w_decay,
    decay_scale,
    decay_bias,
    head_gain,
    w_output,
    ffn_gain,
    route_ids,
    route_weights,
    expert_gate,
    expert_up,
    expert_down,
    shared_gate,
    shared_up,
    shared_down,
):
    rows_count = tokens.shape[0]
    heads_here = delta_state.shape[1]
    tp_index = lax.axis_index("tp")
    core = tp_index % 2
    place = tp_index[None]
    chips = lax.axis_size("tp") // 2
    small = pack_small(w_beta, w_decay, mix_gain, head_gain, decay_scale, decay_bias, ffn_gain)
    own_rows = exchange_chips(jnp.broadcast_to(tokens[None], (chips,) + tokens.shape))
    new_state, kept, sent, full_rows = mixer(
        place, own_rows, swap_cores(own_rows), small, delta_state, w_query, w_key, w_value,
        w_outgate, w_output,
    )
    halves = (kept + swap_cores(sent).astype(jnp.float32)).astype(jnp.bfloat16)
    mixed = sum_chips(halves)
    model_width = full_rows.shape[1]
    ep_count = lax.axis_size("ep")
    tp_count = lax.axis_size("tp")
    experts_here = expert_gate.shape[0]
    top_count = route_ids.shape[1]
    expert_total = experts_here * ep_count * tp_count
    capacity = max(2, 8 * rows_count * top_count // (3 * expert_total))
    pair_count = rows_count * top_count
    flat_ids = route_ids.reshape(pair_count)
    owner_ep = flat_ids // (tp_count * experts_here)
    owner_tp = flat_ids // experts_here % tp_count
    local_slot = flat_ids % experts_here
    mine_mask = owner_tp == tp_index
    pair_weights = jnp.where(mine_mask, route_weights.reshape(pair_count), 0.0)
    pair_index = jnp.arange(pair_count, dtype=jnp.int32)
    earlier = (flat_ids[:, None] == flat_ids[None, :]) & (pair_index[None, :] < pair_index[:, None])
    slot_rank = jnp.sum(earlier.astype(jnp.int32), axis=1)
    slot_count = ep_count * experts_here * capacity
    target = jnp.where(mine_mask, (owner_ep * experts_here + local_slot) * capacity + slot_rank, -1)
    choose = (target[:, None] == jnp.arange(slot_count, dtype=jnp.int32)[None, :]).astype(
        jnp.bfloat16
    )
    by_row = jnp.sum(choose.reshape(rows_count, top_count, slot_count), axis=1)
    outgoing, normed_ffn, resid_own = dispatch(
        place, mixed, swap_cores(mixed), full_rows, small, by_row.T
    )
    outgoing = outgoing.reshape(ep_count, experts_here, capacity, model_width)
    results = expert_block(
        lax.all_to_all(outgoing, "ep", split_axis=0, concat_axis=0, tiled=True),
        expert_gate,
        expert_up,
        expert_down,
    )
    returned = lax.all_to_all(results, "ep", split_axis=0, concat_axis=0, tiled=True)
    weights_of = jnp.sum(
        jnp.where(choose > 0, pair_weights[:, None], 0.0).reshape(rows_count, top_count, slot_count),
        axis=1,
    )
    weights_high = weights_of.astype(jnp.bfloat16)
    weights_low = (weights_of - weights_high.astype(jnp.float32)).astype(jnp.bfloat16)
    returned = returned.reshape(slot_count, model_width)
    routed = jnp.dot(
        jnp.concatenate([weights_high, weights_low], axis=1),
        jnp.concatenate([returned, returned], axis=0),
        preferred_element_type=jnp.float32,
    )
    shared_gate_part = jnp.dot(normed_ffn, shared_gate, preferred_element_type=jnp.float32)
    shared_up_part = jnp.dot(normed_ffn, shared_up, preferred_element_type=jnp.float32)
    hidden_shared = (jax.nn.silu(shared_gate_part) * shared_up_part).astype(jnp.bfloat16)
    branch_sum = routed + jnp.dot(hidden_shared, shared_down, preferred_element_type=jnp.float32)
    combined = scatter_sum(branch_sum, core)
    layer_out = (resid_own + combined).astype(jnp.bfloat16)
    return (layer_out, new_state)


def solution(mesh):
    return jax.shard_map(
        body,
        mesh=mesh,
        in_specs=(
            P("ep", "tp"),
            P("ep", "tp", None, None),
            P(),
            P(None, "tp"),
            P(None, "tp"),
            P(None, "tp"),
            P(None, "tp"),
            P(None, "tp"),
            P(None, "tp"),
            P("tp"),
            P("tp"),
            P(),
            P("tp", None),
            P(),
            P("ep", None),
            P("ep", None),
            P(("ep", "tp"), None, None),
            P(("ep", "tp"), None, None),
            P(("ep", "tp"), None, None),
            P(None, "tp"),
            P(None, "tp"),
            P("tp", None),
        ),
        out_specs=(P("ep", "tp"), P("ep", "tp", None, None)),
        check_vma=False,
    )
```
